32 devices in a mesh: rep: 8 (over z, y), fs: 2 (over core), tp: 2 (over x).
Axes of the slice: x: 2, y: 2, z: 4, core: 2. Of those that a mesh axis runs over, the one named last changes fastest.
Arguments:
- inputs: bfloat16 [2048, 2048], P(('rep', 'fs'), 'tp'), may hold values from -6 to 6
- cotangent: bfloat16 [2048, 2048], P(('rep', 'fs'), 'tp'), may hold values from -6 to 6
- w_up: bfloat16 [2048, 4096], P('fs', 'tp'), may hold values from -0.125 to 0.125
- w_down: bfloat16 [4096, 2048], P('tp', 'fs'), may hold values from -0.09375 to 0.09375
Outputs:
- grad_inputs: bfloat16 [2048, 2048], P(('rep', 'fs'), 'tp')
- grad_up: float32 [2048, 4096], P('fs', 'tp')
- grad_down: float32 [4096, 2048], P('tp', 'fs')
The draws below stay inside these ranges and needn't reach their ends.
All inputs are finite; a program needn't handle non-finite values.
Results may differ from the reference program's by a relative error of at most 0.011.
Values may be sent and summed in bfloat16 or wider, within the bound.
No kernel may reach another device: no remote copies, remote signals or barrier semaphores. Data moves between devices by JAX's collectives and lax.ppermute only.
A program may use at most 128 MiB of HBM per device.

```python
import jax
import jax.numpy as jnp
from jax import lax

D = 2048
FF = 4096
TOKENS = 2048
N_TP = 2


def raised(entries, key, source, target, parts, factor):
    owner, partner = [(jnp.arange(entries.shape[axis_at]) // (entries.shape[axis_at] // parts)).reshape([-1 if axis == axis_at else 1 for axis in range(entries.ndim)]) for axis_at in (source, target)]
    chosen = jax.random.permutation(key, parts)[partner]
    strong = (owner == chosen) | (owner == (partner + parts // 2) % parts)
    return jnp.where(strong, factor * entries, entries)


def levels(own_key, shape, pieces, low, largest):
    def one(position, shards_of):
        heights = jax.random.uniform(jax.random.fold_in(jax.random.fold_in(own_key, 6), position), (shards_of,), jnp.float32, low / len(pieces), largest / len(pieces))
        return jnp.repeat(jnp.exp(heights), shape[position] // shards_of).reshape((-1,) + (1,) * (len(shape) - position - 1))

    loudness = one(*pieces[0])
    for cut in pieces[1:]:
        loudness = loudness * one(*cut)
    return loudness


def normal_values(rng, shape, width, most, split=(), dtype=jnp.bfloat16):
    entries = jax.random.normal(rng, shape, jnp.float32) * width
    if len(split) > 0:
        entries = levels(rng, shape, split, -0.22, 0.18) * entries
    return jnp.clip(entries, min=-most, max=most).astype(dtype)


def bell_draw_with(rng, extent, deviation, limit, cuts, heavy, dtype=jnp.bfloat16):
    values = deviation * jax.random.normal(rng, extent, jnp.float32)
    if cuts:
        values = values * levels(rng, extent, cuts, -0.22, 0.18)
    return jnp.clip(raised(values, jax.random.fold_in(rng, 3), *heavy), -limit, limit).astype(dtype)


def setup_inputs(seed: int = 0) -> dict:
    arg_keys = jax.random.split(jax.random.key(seed), 5)
    return {
        "inputs": bell_draw_with(arg_keys[0], (TOKENS, D), 1.0, 6.0, ((0, 16), (1, 2)), (0, 1, 16, 2.0)),
        "cotangent": bell_draw_with(arg_keys[1], (TOKENS, D), 1.0, 6.0, ((0, 16), (1, 2)), (0, 1, 16, 2.0)),
        "w_up": normal_values(arg_keys[2], (D, FF), D ** -0.5, 0.125, ((0, 2), (1, 2))),
        "w_down": normal_values(arg_keys[3], (FF, D), FF ** -0.5, 0.09375, ((0, 2), (1, 2))),
    }


def reference(inputs, cotangent, w_up, w_down):
    preact = jnp.dot(inputs, w_up, preferred_element_type=jnp.float32)
    relu_pre = jnp.maximum(preact, 0.0)
    squared = (relu_pre * relu_pre).astype(jnp.bfloat16)
    act_grad = jnp.dot(cotangent, w_down.T, preferred_element_type=jnp.float32)
    pre_grad = (2.0 * relu_pre * act_grad).astype(jnp.bfloat16)
    grad_up = jnp.dot(inputs.T, pre_grad, preferred_element_type=jnp.float32)
    grad_down = jnp.dot(squared.T, cotangent, preferred_element_type=jnp.float32)
    group = w_up.shape[1] // N_TP
    total = jnp.zeros(inputs.shape, jnp.float32)
    for index in range(N_TP):
        partial_value = jnp.dot(pre_grad[:, index * group:(index + 1) * group],
                          w_up[:, index * group:(index + 1) * group].T,
                          preferred_element_type=jnp.float32).astype(jnp.bfloat16)
        partial_value = lax.optimization_barrier(partial_value)
        total = total + partial_value.astype(jnp.float32)
    return total.astype(jnp.bfloat16), grad_up, grad_down
```

```python
import jax
import jax.numpy as jnp
from jax import lax
from jax.sharding import PartitionSpec as P


def contract_rows(left, right):
    return lax.dot_general(
        left, right, (((0,), (0,)), ((), ())), preferred_element_type=jnp.float32
    )


def contract_cols(left, right):
    return lax.dot_general(
        left, right, (((1,), (1,)), ((), ())), preferred_element_type=jnp.float32
    )


def folded_ring(length):
    return [0] + list(range(1, length, 2)) + list(range(length - 2 + length % 2, 0, -2))


def plan(n_rep, tokens_each, width, hidden):
    group = n_rep
    while group > 2 and (n_rep % group or group % 2 or group * tokens_each > hidden):
        group -= 1
    return group


def build(mesh):
    n_rep, n_fs, n_tp = (mesh.shape[name] for name in ("rep", "fs", "tp"))

    def shards(inputs, cotangent, w_up, w_down):
        rows, part = inputs.shape
        group = plan(n_rep, rows * n_fs, part * n_tp, w_up.shape[1])
        length = group // 2
        ring = folded_ring(length)
        follows = {ring[i]: ring[(i + 1) % length] for i in range(length)}
        along = [
            (base * group + 2 * at + side, base * group + 2 * follows[at] + side)
            for base in range(n_rep // group)
            for at in range(length)
            for side in range(2)
        ]
        across = [(place, place ^ 1) for place in range(n_rep)]
        swap = [(0, 1), (1, 0)]
        same = lax.axis_index("fs") == lax.axis_index("tp")

        other_up = lax.ppermute(w_up, "fs", swap)
        other_down = lax.ppermute(w_down, "fs", swap)
        near = jnp.stack([inputs, cotangent])
        sums = None
        held = []
        for step in range(length):
            beside = lax.ppermute(near, "tp", swap)
            over = lax.ppermute(near, "rep", across)
            if step + 1 < length:
                following = lax.ppermute(near, "rep", along)
            corner_in = lax.ppermute(over[0], "tp", swap)
            corner_cot = lax.ppermute(beside[1], "rep", across)
            mine = jnp.concatenate([near, over], axis=1)
            theirs = jnp.concatenate([beside, jnp.stack([corner_in, corner_cot])], axis=1)
            if step == 0:
                full_up = jnp.concatenate(
                    [jnp.where(same, w_up, other_up), jnp.where(same, other_up, w_up)], axis=0
                )
                full_down = jnp.concatenate(
                    [jnp.where(same, w_down, other_down), jnp.where(same, other_down, w_down)], axis=1
                )
            whole = jnp.concatenate([mine, theirs], axis=2)
            preact = jnp.dot(whole[0], full_up, preferred_element_type=jnp.float32)
            relu_pre = jnp.maximum(preact, 0.0)
            act_grad = contract_cols(whole[1], full_down)
            squared = (relu_pre * relu_pre).astype(jnp.bfloat16)
            pre_grad = (2.0 * relu_pre * act_grad).astype(jnp.bfloat16)
            if step == 0:
                partial_value = contract_cols(pre_grad[:rows], full_up).astype(jnp.bfloat16)
                passed = lax.ppermute(partial_value[:, part:], "tp", swap)
                grad_inputs = (
                    partial_value[:, :part].astype(jnp.float32) + passed.astype(jnp.float32)
                ).astype(jnp.bfloat16)
            keep = jnp.where(same, mine, theirs)
            give = jnp.where(same, theirs, mine)
            got = lax.ppermute(give, "fs", swap)
            hidden = jnp.stack([pre_grad, squared])
            got_hidden = lax.ppermute(hidden, "fs", swap)
            held.append((keep, got, hidden, got_hidden))
            if step >= length - 2:
                cols = jnp.concatenate([t for h in held for t in h[:2]], axis=1)
                hid = jnp.concatenate([t for h in held for t in h[2:]], axis=1)
                held = []
                new = contract_rows(cols[0], hid[0]), contract_rows(hid[1], cols[1])
                sums = new if sums is None else (sums[0] + new[0], sums[1] + new[1])
            if step + 1 < length:
                near = following
        grad_up, grad_down = sums
        if n_rep > group:
            groups = [
                [base * group + at for base in range(n_rep // group)] for at in range(group)
            ]
            grad_up, grad_down = (
                lax.psum(t, "rep", axis_index_groups=groups) for t in (grad_up, grad_down)
            )
        return (grad_inputs, grad_up, grad_down)

    return shards


def solution(mesh):
    return jax.shard_map(
        build(mesh),
        mesh=mesh,
        in_specs=(P(("rep", "fs"), "tp"), P(("rep", "fs"), "tp"), P("fs", "tp"), P("tp", "fs")),
        out_specs=(P(("rep", "fs"), "tp"), P("fs", "tp"), P("tp", "fs")),
        check_vma=False,
    )
```

```python
import functools

import jax
import jax.numpy as jnp
from jax import lax
from jax.experimental import pallas as pl
from jax.experimental.pallas import tpu as pltpu
from jax.sharding import PartitionSpec as P


BF16, F32 = jnp.bfloat16, jnp.float32
VMEM = pl.BlockSpec(memory_space=pltpu.VMEM)
SMEM = pl.BlockSpec(memory_space=pltpu.SMEM)
HBM = pl.BlockSpec(memory_space=pltpu.HBM)
MIB = 1 << 20


def dot(left, right, contract):
    return lax.dot_general(left, right, (contract, ((), ())), preferred_element_type=F32)


def tile_of(size):
    return 512 if size % 512 == 0 else size


def folded_ring(length):
    return [0] + list(range(1, length, 2)) + list(range(length - 2 + length % 2, 0, -2))


def plan(n_rep, tokens_each, hidden):
    group = n_rep
    while group > 2 and (n_rep % group or group % 2 or group * tokens_each > hidden):
        group -= 1
    return group


def ready_kernel(flag_ref, up_ref, down_ref, out_ref):
    out_ref[0] = flag_ref[0]


def ready(flag, w_up, w_down):
    return pl.pallas_call(
        ready_kernel,
        in_specs=[SMEM, VMEM, VMEM],
        out_specs=SMEM,
        out_shape=jax.ShapeDtypeStruct((1,), jnp.int32),
        compiler_params=pltpu.CompilerParams(vmem_limit_bytes=10 * MIB),
        name="ready",
    )(flag, w_up, w_down)


def forward_kernel(count, first, same_ref, *refs):
    mine, theirs = refs[:count], refs[count : 2 * count]
    up_ref, down_ref, up_other, down_other = refs[2 * count : 2 * count + 4]
    packet_ref, keep_ref, *part_ref = refs[2 * count + 4 : 2 * count + 6 + first]
    give_ref, up_buf, down_buf, sems, *sum_ref = refs[2 * count + 6 + first :]
    _, rows, _ = mine[0].shape
    hidden, tile = up_ref.shape[1], up_buf.shape[2]
    steps = hidden // tile

    def copy(step, which):
        slot = lax.rem(step, 2)
        cols = pl.ds(pl.multiple_of(step * tile, tile), tile)
        if which == 0:
            source, target = up_other.at[:, cols], up_buf.at[slot]
        else:
            source, target = down_other.at[cols, :], down_buf.at[slot]
        return pltpu.make_async_copy(source, target, sems.at[slot, which])

    for which in range(2):
        copy(0, which).start()

    def choose(kept, given):
        for at in range(count):
            place = pl.ds(at * rows, rows)
            keep_ref[:, place, :] = kept[at][...]
            give_ref[:, place, :] = given[at][...]
            packet_ref[:, place, hidden:] = given[at][...]

    if first:
        sum_ref[0][...] = jnp.zeros_like(sum_ref[0])
    same = same_ref[0] == 1

    @pl.when(same)
    def _():
        choose(mine, theirs)

    @pl.when(jnp.logical_not(same))
    def _():
        choose(theirs, mine)

    @pl.loop(0, steps)
    def _(step):
        slot = lax.rem(step, 2)
        cols = pl.ds(pl.multiple_of(step * tile, tile), tile)

        @pl.when(step + 1 < steps)
        def _():
            for which in range(2):
                copy(step + 1, which).start()

        for which in range(2):
            copy(step, which).wait()
        preact = dot(keep_ref[0], up_ref[:, cols], ((1,), (0,)))
        preact += dot(give_ref[0], up_buf[slot], ((1,), (0,)))
        act_grad = dot(keep_ref[1], down_ref[cols, :], ((1,), (1,)))
        act_grad += dot(give_ref[1], down_buf[slot], ((1,), (1,)))
        relu_pre = jnp.maximum(preact, 0.0)
        pre_grad = (2.0 * relu_pre * act_grad).astype(BF16)
        packet_ref[0, :, cols] = pre_grad
        packet_ref[1, :, cols] = (relu_pre * relu_pre).astype(BF16)
        if first:
            for at, held in enumerate((up_ref[:, cols], up_buf[slot])):
                sum_ref[0][at] += dot(pre_grad[:rows], held, ((1,), (1,)))

    if first:
        part_ref[0][1 - same_ref[0]] = sum_ref[0][0].astype(BF16)
        part_ref[0][same_ref[0]] = sum_ref[0][1].astype(BF16)


def forward(same, mine, theirs, weights, first):
    count = len(mine)
    _, rows, part = mine[0].shape
    hidden = weights[0].shape[1]
    tokens, tile = count * rows, tile_of(hidden)
    return pl.pallas_call(
        functools.partial(forward_kernel, count, first),
        in_specs=[SMEM] + [VMEM] * (2 * count + 2) + [HBM] * 2,
        out_specs=[VMEM] * (2 + first),
        out_shape=[
            jax.ShapeDtypeStruct((2, tokens, hidden + part), BF16),
            jax.ShapeDtypeStruct((2, tokens, part), BF16),
            jax.ShapeDtypeStruct((2, rows, part), BF16),
        ][: 2 + first],
        scratch_shapes=[
            pltpu.VMEM((2, tokens, part), BF16),
            pltpu.VMEM((2, part, tile), BF16),
            pltpu.VMEM((2, tile, part), BF16),
            pltpu.SemaphoreType.DMA((2, 2)),
            pltpu.VMEM((2, rows, part), F32),
        ][: 4 + first],
        compiler_params=pltpu.CompilerParams(vmem_limit_bytes=11 * MIB),
        cost_estimate=pl.CostEstimate(
            flops=8 * tokens * part * hidden, bytes_accessed=8 * part * hidden, transcendentals=0
        ),
        name="forward",
    )(same, *mine, *theirs, *weights)


def grads_of(pieces, cols, hidden):
    def rows(which):
        parts = []
        for keep, packet, got in pieces:
            parts += [packet[which, :, cols], got[which, :, cols]]
        return jnp.concatenate(parts, axis=0)

    def tokens(which):
        parts = []
        for keep, packet, got in pieces:
            parts += [keep[which], got[which, :, hidden:]]
        return jnp.concatenate(parts, axis=0)

    up = dot(tokens(0), rows(0), ((0,), (0,)))
    return up, dot(rows(1), tokens(1), ((0,), (0,)))


def triples(refs, count):
    return [refs[3 * at : 3 * at + 3] for at in range(count)]


def accumulate_kernel(count, first, last, *refs):
    pieces = triples(refs, count)
    up_ref, down_ref = refs[-2:]
    up_in, down_in = (None, None) if first else refs[3 * count : 3 * count + 2]
    hidden = down_ref.shape[0] if first else down_in.shape[0]
    tile = down_ref.shape[0] if last else tile_of(hidden)

    def add(step, up_to, down_to):
        cols = pl.ds(pl.multiple_of(step * tile, tile), tile)
        up, down = grads_of(pieces, cols, hidden)
        if not first:
            up, down = up_in[:, cols].astype(F32) + up, down_in[cols, :].astype(F32) + down
        up_ref[:, up_to(cols)] = up.astype(up_ref.dtype)
        down_ref[down_to(cols), :] = down.astype(down_ref.dtype)

    if last:
        add(pl.program_id(0), lambda cols: slice(None), lambda cols: slice(None))
    else:
        pl.loop(0, hidden // tile)(lambda step: add(step, lambda cols: cols, lambda cols: cols))


def accumulate(pieces, sums, last):
    keep, packet, _ = pieces[0]
    tokens = sum(piece[0].shape[1] for piece in pieces)
    part = keep.shape[2]
    hidden = packet.shape[2] - part
    tile = tile_of(hidden)
    args = [array for piece in pieces for array in piece] + list(sums or ())
    how = dict(
        in_specs=[VMEM] * len(args),
        out_specs=[VMEM, VMEM],
        out_shape=[
            jax.ShapeDtypeStruct((part, hidden), F32 if last else BF16),
            jax.ShapeDtypeStruct((hidden, part), F32 if last else BF16),
        ],
        compiler_params=pltpu.CompilerParams(vmem_limit_bytes=(16 if last else 9) * MIB),
        cost_estimate=pl.CostEstimate(
            flops=8 * tokens * part * hidden, bytes_accessed=8 * part * hidden, transcendentals=0
        ),
        name="accumulate",
    )
    if last:
        how |= dict(
            grid=(hidden // tile,),
            out_specs=[
                pl.BlockSpec((part, tile), lambda j: (0, j)),
                pl.BlockSpec((tile, part), lambda j: (j, 0)),
            ],
        )
    elif sums is not None:
        how |= dict(input_output_aliases={len(args) - 2: 0, len(args) - 1: 1})
    return pl.pallas_call(
        functools.partial(accumulate_kernel, len(pieces), sums is None, last), **how
    )(*args)


def build(mesh):
    n_rep, n_fs, _ = (mesh.shape[name] for name in ("rep", "fs", "tp"))

    def shards(inputs, cotangent, w_up, w_down):
        rows, _ = inputs.shape
        group = plan(n_rep, rows * n_fs, w_up.shape[1])
        length = group // 2
        ring = folded_ring(length)
        follows = {ring[i]: ring[(i + 1) % length] for i in range(length)}
        along = [
            (base * group + 2 * at + side, base * group + 2 * follows[at] + side)
            for base in range(n_rep // group)
            for at in range(length)
            for side in range(2)
        ]
        back = [(target, source) for source, target in along]
        across = [(place, place ^ 1) for place in range(n_rep)]
        swap = [(0, 1), (1, 0)]

        same = lax.axis_index("fs") == lax.axis_index("tp")
        flag = same.astype(jnp.int32)[None]

        near = [jnp.stack([inputs, cotangent])]
        beside, over, corner = [], [], {}
        other_up = lax.ppermute(w_up, "fs", swap)
        other_down = lax.ppermute(w_down, "fs", swap)
        weights = (w_up, w_down, other_up, other_down)
        flag = ready(flag, w_up, w_down)
        for step in range(length):
            beside.append(lax.ppermute(near[step], "tp", swap))
            over.append(lax.ppermute(near[step], "rep", across))
            if step == 0:
                corner[0] = lax.ppermute(beside[0], "rep", across)
            if step + 1 < length:
                near.append(lax.ppermute(near[step], "rep", along))
        for step in range(length - 1, 1, -1):
            corner[step] = lax.ppermute(corner[(step + 1) % length], "rep", back)
        if length > 1:
            corner[1] = lax.ppermute(over[1], "tp", swap)
        own = [(near[k], beside[k]) for k in range(length)]
        far = [(over[k], corner[k]) for k in range(length)]
        groups = {f"o{k}": group for k, group in enumerate(own)}
        groups |= {f"f{k}": group for k, group in enumerate(far)}

        made = []
        for at, names in enumerate(CHUNKS):
            packet, keep, *partial_value = forward(
                flag, *zip(*(groups[name] for name in names)), weights, at == 0
            )
            if at == 0:
                partial_here, partial_there = partial_value[0]
            made.append((keep, packet, lax.ppermute(packet, "fs", swap)))
        sums = None
        for at, chunks in enumerate(BATCHES):
            sums = accumulate([made[k] for k in chunks], sums, at == len(BATCHES) - 1)
        grad_up, grad_down = sums

        passed = lax.ppermute(partial_there, "tp", swap)
        grad_inputs = (partial_here.astype(F32) + passed.astype(F32)).astype(BF16)
        if n_rep > group:
            sets = [[base * group + at for base in range(n_rep // group)] for at in range(group)]
            grad_up, grad_down = (
                lax.psum(t, "rep", axis_index_groups=sets) for t in (grad_up, grad_down)
            )
        return (grad_inputs, grad_up, grad_down)

    return shards


CHUNKS = (("o0",), ("o1", "f0"), ("o2", "o3"), ("f3", "f1", "f2"))
BATCHES = ((0, 1), (2,), (3,))


def solution(mesh):
    run = build(mesh)

    return jax.shard_map(
        run,
        mesh=mesh,
        in_specs=(P(("rep", "fs"), "tp"), P(("rep", "fs"), "tp"), P("fs", "tp"), P("tp", "fs")),
        out_specs=(P(("rep", "fs"), "tp"), P("fs", "tp"), P("tp", "fs")),
        check_vma=False,
    )
```

```python
import functools

import jax
import jax.numpy as jnp
from jax import lax
from jax.experimental import pallas as pl
from jax.experimental.pallas import tpu as pltpu
from jax.sharding import PartitionSpec as P


BF16, F32 = jnp.bfloat16, jnp.float32
VMEM = pl.BlockSpec(memory_space=pltpu.VMEM)
SMEM = pl.BlockSpec(memory_space=pltpu.SMEM)
HBM = pl.BlockSpec(memory_space=pltpu.HBM)
MIB = 1 << 20
FORWARD_MIB = 5


def dot(left, right, contract):
    return lax.dot_general(left, right, (contract, ((), ())), preferred_element_type=F32)


def tile_of(size):
    return 512 if size % 512 == 0 else size


def folded_ring(length):
    return [0] + list(range(1, length, 2)) + list(range(length - 2 + length % 2, 0, -2))


def plan(n_rep, tokens_each, hidden):
    group = n_rep
    while group > 2 and (n_rep % group or group % 2 or group * tokens_each > hidden):
        group -= 1
    return group


def ready_kernel(flag_ref, up_ref, down_ref, out_ref):
    out_ref[0] = flag_ref[0]


def ready(flag, w_up, w_down):
    return pl.pallas_call(
        ready_kernel,
        in_specs=[SMEM, VMEM, VMEM],
        out_specs=SMEM,
        out_shape=jax.ShapeDtypeStruct((1,), jnp.int32),
        compiler_params=pltpu.CompilerParams(vmem_limit_bytes=10 * MIB),
        name="ready",
    )(flag, w_up, w_down)


def forward_kernel(count, first, same_ref, *refs):
    mine, theirs = refs[:count], refs[count : 2 * count]
    up_ref, down_ref, up_other, down_other, packet_ref, keep_ref, *rest = refs[2 * count :]
    _, rows, _ = mine[0].shape
    hidden = up_ref.shape[1]
    tile = tile_of(hidden)
    steps = hidden // tile
    if first:
        up_held, down_held, give_ref, sems = rest
        sources, up_other, down_other = (up_other, down_other), up_held, down_held

        def copies(step):
            cols = pl.ds(pl.multiple_of(step * tile, tile), tile)
            return (
                pltpu.make_async_copy(sources[0].at[:, cols], up_held.at[:, cols], sems.at[0, step]),
                pltpu.make_async_copy(sources[1].at[cols, :], down_held.at[cols, :], sems.at[1, step]),
            )

        for step in range(steps):
            for copy in copies(step):
                copy.start()
    else:
        (give_ref,) = rest

    def choose(kept, given):
        for at in range(count):
            place = pl.ds(at * rows, rows)
            keep_ref[:, place, :] = kept[at][...]
            give_ref[:, place, :] = given[at][...]
            packet_ref[:, place, hidden:] = given[at][...]

    same = same_ref[0] == 1

    @pl.when(same)
    def _():
        choose(mine, theirs)

    @pl.when(jnp.logical_not(same))
    def _():
        choose(theirs, mine)

    @pl.loop(0, steps)
    def _(step):
        cols = pl.ds(pl.multiple_of(step * tile, tile), tile)
        if first:
            for copy in copies(step):
                copy.wait()
        preact = dot(keep_ref[0], up_ref[:, cols], ((1,), (0,)))
        preact += dot(give_ref[0], up_other[:, cols], ((1,), (0,)))
        act_grad = dot(keep_ref[1], down_ref[cols, :], ((1,), (1,)))
        act_grad += dot(give_ref[1], down_other[cols, :], ((1,), (1,)))
        relu_pre = jnp.maximum(preact, 0.0)
        packet_ref[0, :, cols] = (2.0 * relu_pre * act_grad).astype(BF16)
        packet_ref[1, :, cols] = (relu_pre * relu_pre).astype(BF16)


def forward(same, mine, theirs, weights, first):
    count = len(mine)
    _, rows, part = mine[0].shape
    hidden = weights[0].shape[1]
    tokens = count * rows
    made = [
        jax.ShapeDtypeStruct((2, tokens, hidden + part), BF16),
        jax.ShapeDtypeStruct((2, tokens, part), BF16),
    ]
    scratch = [pltpu.VMEM((2, tokens, part), BF16)]
    if first:
        made += [jax.ShapeDtypeStruct(t.shape, t.dtype) for t in weights[2:]]
        scratch += [pltpu.SemaphoreType.DMA((2, hidden // tile_of(hidden)))]
    return pl.pallas_call(
        functools.partial(forward_kernel, count, first),
        in_specs=[SMEM] + [VMEM] * (2 * count + 2) + [HBM if first else VMEM] * 2,
        out_specs=[VMEM] * len(made),
        out_shape=made,
        scratch_shapes=scratch,
        compiler_params=pltpu.CompilerParams(vmem_limit_bytes=FORWARD_MIB * MIB),
        cost_estimate=pl.CostEstimate(
            flops=8 * tokens * part * hidden, bytes_accessed=8 * part * hidden, transcendentals=0
        ),
        name="forward",
    )(same, *mine, *theirs, *weights)


def inputs_kernel(same_ref, packet_ref, up_ref, up_other, out_ref):
    _, rows, part = out_ref.shape
    tile = tile_of(part)
    pre_grad = packet_ref[0, :rows, : up_ref.shape[1]]
    same = same_ref[0]
    for held, here in ((up_ref, 1 - same), (up_other, same)):
        for at in range(0, part, tile):
            place = pl.ds(at, tile)
            out_ref[here, :, place] = dot(pre_grad, held[place, :], ((1,), (1,))).astype(BF16)


def inputs_part(same, packet, rows, held_up, other_up):
    part, hidden = held_up.shape
    return pl.pallas_call(
        inputs_kernel,
        in_specs=[SMEM] + [VMEM] * 3,
        out_specs=VMEM,
        out_shape=jax.ShapeDtypeStruct((2, rows, part), BF16),
        compiler_params=pltpu.CompilerParams(vmem_limit_bytes=FORWARD_MIB * MIB),
        cost_estimate=pl.CostEstimate(
            flops=4 * rows * part * hidden, bytes_accessed=4 * part * hidden, transcendentals=0
        ),
        name="inputs_part",
    )(same, packet, held_up, other_up)


def grads_of(pieces, cols, hidden):
    def rows(which):
        parts = []
        for keep, packet, got in pieces:
            parts += [packet[which, :, cols], got[which, :, cols]]
        return jnp.concatenate(parts, axis=0)

    def tokens(which):
        parts = []
        for keep, packet, got in pieces:
            parts += [keep[which], got[which, :, hidden:]]
        return jnp.concatenate(parts, axis=0)

    return lambda: dot(tokens(0), rows(0), ((0,), (0,))), lambda: dot(rows(1), tokens(1), ((0,), (0,)))


def triples(refs, count):
    return [refs[3 * at : 3 * at + 3] for at in range(count)]


def accumulate_kernel(count, first, last, *refs):
    pieces = triples(refs, count)
    up_ref, down_ref = refs[-2:]
    up_in, down_in = (None, None) if first else refs[3 * count : 3 * count + 2]
    hidden = down_ref.shape[0] if first else down_in.shape[0]
    tile = down_ref.shape[0] if last else tile_of(hidden)

    def add(step, up_to, down_to):
        cols = pl.ds(pl.multiple_of(step * tile, tile), tile)
        up, down = grads_of(pieces, cols, hidden)
        total = up() if first else up_in[:, cols].astype(F32) + up()
        up_ref[:, up_to(cols)] = total.astype(up_ref.dtype)
        total = down() if first else down_in[cols, :].astype(F32) + down()
        down_ref[down_to(cols), :] = total.astype(down_ref.dtype)

    if last:
        add(pl.program_id(0), lambda cols: slice(None), lambda cols: slice(None))
    else:
        pl.loop(0, hidden // tile)(lambda step: add(step, lambda cols: cols, lambda cols: cols))


def accumulate(pieces, sums, last):
    keep, packet, _ = pieces[0]
    tokens = sum(piece[0].shape[1] for piece in pieces)
    part = keep.shape[2]
    hidden = packet.shape[2] - part
    tile = tile_of(hidden)
    args = [array for piece in pieces for array in piece] + list(sums or ())
    how = dict(
        in_specs=[VMEM] * len(args),
        out_specs=[VMEM, VMEM],
        out_shape=[
            jax.ShapeDtypeStruct((part, hidden), F32 if last else BF16),
            jax.ShapeDtypeStruct((hidden, part), F32 if last else BF16),
        ],
        compiler_params=pltpu.CompilerParams(vmem_limit_bytes=(12 if last else 7) * MIB),
        cost_estimate=pl.CostEstimate(
            flops=8 * tokens * part * hidden, bytes_accessed=8 * part * hidden, transcendentals=0
        ),
        name="accumulate",
    )
    if last:
        how |= dict(
            grid=(hidden // tile,),
            out_specs=[
                pl.BlockSpec((part, tile), lambda j: (0, j)),
                pl.BlockSpec((tile, part), lambda j: (j, 0)),
            ],
        )
    elif sums is not None:
        how |= dict(input_output_aliases={len(args) - 2: 0, len(args) - 1: 1})
    return pl.pallas_call(
        functools.partial(accumulate_kernel, len(pieces), sums is None, last), **how
    )(*args)


def build(mesh):
    n_rep, n_fs, _ = (mesh.shape[name] for name in ("rep", "fs", "tp"))

    def shards(inputs, cotangent, w_up, w_down):
        rows, _ = inputs.shape
        group = plan(n_rep, rows * n_fs, w_up.shape[1])
        length = group // 2
        ring = folded_ring(length)
        follows = {ring[i]: ring[(i + 1) % length] for i in range(length)}
        along = [
            (base * group + 2 * at + side, base * group + 2 * follows[at] + side)
            for base in range(n_rep // group)
            for at in range(length)
            for side in range(2)
        ]
        back = [(target, source) for source, target in along]
        across = [(place, place ^ 1) for place in range(n_rep)]
        swap = [(0, 1), (1, 0)]

        same = lax.axis_index("fs") == lax.axis_index("tp")
        flag = same.astype(jnp.int32)[None]

        far_end = length - 1 if length > 2 else None
        near = {0: jnp.stack([inputs, cotangent])}
        beside = {0: lax.ppermute(near[0], "tp", swap)}
        over = {0: lax.ppermute(near[0], "rep", across)}
        corner = {0: lax.ppermute(beside[0], "rep", across)}
        for step in range(1, length):
            near[step] = lax.ppermute(near[step - 1], "rep", along)
            if step == far_end:
                beside[step] = lax.ppermute(beside[0], "rep", back)
                over[step] = lax.ppermute(over[0], "rep", back)
                corner[step] = lax.ppermute(beside[step], "rep", across)
            else:
                beside[step] = lax.ppermute(near[step], "tp", swap)
                over[step] = lax.ppermute(near[step], "rep", across)
                corner[step] = lax.ppermute(over[step], "tp", swap)
        other_up = lax.ppermute(w_up, "fs", swap)
        other_down = lax.ppermute(w_down, "fs", swap)
        weights = (w_up, w_down, other_up, other_down)
        flag = ready(flag, w_up, w_down)
        own = [(near[k], beside[k]) for k in range(length)]
        far = [(over[k], corner[k]) for k in range(length)]
        groups = {f"o{k}": group for k, group in enumerate(own)}
        groups |= {f"f{k}": group for k, group in enumerate(far)}

        made = []
        for at, names in enumerate(CHUNKS):
            packet, keep, *more = forward(
                flag, *zip(*(groups[name] for name in names)), weights, at == 0
            )
            if at == 0:
                weights = (w_up, w_down, *more)
            made.append((keep, packet, lax.ppermute(packet, "fs", swap)))
        sums = None
        for at, chunks in enumerate(BATCHES):
            sums = accumulate([made[k] for k in chunks], sums, at == len(BATCHES) - 1)
        grad_up, grad_down = sums

        partial_value = inputs_part(flag, made[0][1], rows, w_up, weights[2])
        passed = lax.ppermute(partial_value[1], "tp", swap)
        grad_inputs = (partial_value[0].astype(F32) + passed.astype(F32)).astype(BF16)
        if n_rep > group:
            sets = [[base * group + at for base in range(n_rep // group)] for at in range(group)]
            grad_up, grad_down = (
                lax.psum(t, "rep", axis_index_groups=sets) for t in (grad_up, grad_down)
            )
        return (grad_inputs, grad_up, grad_down)

    return shards


CHUNKS = (("o0",), ("o1", "f0"), ("o2", "f1", "o3"), ("f2", "f3"))
BATCHES = ((0, 1), (2,), (3,))


def solution(mesh):
    run = build(mesh)

    return jax.shard_map(
        run,
        mesh=mesh,
        in_specs=(P(("rep", "fs"), "tp"), P(("rep", "fs"), "tp"), P("fs", "tp"), P("tp", "fs")),
        out_specs=(P(("rep", "fs"), "tp"), P("fs", "tp"), P("tp", "fs")),
        check_vma=False,
    )
```

```python
import functools

import jax
import jax.numpy as jnp
from jax import lax
from jax.experimental import pallas as pl
from jax.experimental.pallas import tpu as pltpu
from jax.sharding import PartitionSpec as P


BF16, F32 = jnp.bfloat16, jnp.float32
VMEM = pl.BlockSpec(memory_space=pltpu.VMEM)
SMEM = pl.BlockSpec(memory_space=pltpu.SMEM)
HBM = pl.BlockSpec(memory_space=pltpu.HBM)
MIB = 1 << 20
FORWARD_MIB = 5


def dot(left, right, contract):
    return lax.dot_general(left, right, (contract, ((), ())), preferred_element_type=F32)


def tile_of(size):
    return 512 if size % 512 == 0 else size


def folded_ring(length):
    return [0] + list(range(1, length, 2)) + list(range(length - 2 + length % 2, 0, -2))


def plan(n_rep, tokens_each, hidden):
    group = n_rep
    while group > 2 and (n_rep % group or group % 2 or group * tokens_each > hidden):
        group -= 1
    return group


def ready_kernel(flag_ref, up_ref, down_ref, out_ref):
    out_ref[0] = flag_ref[0]


def ready(flag, w_up, w_down):
    return pl.pallas_call(
        ready_kernel,
        in_specs=[SMEM, VMEM, VMEM],
        out_specs=SMEM,
        out_shape=jax.ShapeDtypeStruct((1,), jnp.int32),
        compiler_params=pltpu.CompilerParams(vmem_limit_bytes=10 * MIB),
        name="ready",
    )(flag, w_up, w_down)


def forward_kernel(count, first, same_ref, *refs):
    mine, theirs = refs[:count], refs[count : 2 * count]
    up_ref, down_ref, up_other, down_other, packet_ref, keep_ref, *rest = refs[2 * count :]
    _, rows, _ = mine[0].shape
    hidden = up_ref.shape[1]
    tile = tile_of(hidden)
    steps = hidden // tile
    if first:
        up_held, down_held, give_ref, sems = rest
        sources, up_other, down_other = (up_other, down_other), up_held, down_held

        def copies(step):
            cols = pl.ds(pl.multiple_of(step * tile, tile), tile)
            return (
                pltpu.make_async_copy(sources[0].at[:, cols], up_held.at[:, cols], sems.at[0, step]),
                pltpu.make_async_copy(sources[1].at[cols, :], down_held.at[cols, :], sems.at[1, step]),
            )

        for step in range(steps):
            for copy in copies(step):
                copy.start()
    else:
        (give_ref,) = rest

    def choose(kept, given):
        for at in range(count):
            place = pl.ds(at * rows, rows)
            keep_ref[:, place, :] = kept[at][...]
            give_ref[:, place, :] = given[at][...]
            packet_ref[:, place, hidden:] = given[at][...]

    same = same_ref[0] == 1

    @pl.when(same)
    def _():
        choose(mine, theirs)

    @pl.when(jnp.logical_not(same))
    def _():
        choose(theirs, mine)

    @pl.loop(0, steps)
    def _(step):
        cols = pl.ds(pl.multiple_of(step * tile, tile), tile)
        if first:
            for copy in copies(step):
                copy.wait()
        preact = dot(keep_ref[0], up_ref[:, cols], ((1,), (0,)))
        preact += dot(give_ref[0], up_other[:, cols], ((1,), (0,)))
        act_grad = dot(keep_ref[1], down_ref[cols, :], ((1,), (1,)))
        act_grad += dot(give_ref[1], down_other[cols, :], ((1,), (1,)))
        relu_pre = jnp.maximum(preact, 0.0)
        packet_ref[0, :, cols] = (2.0 * relu_pre * act_grad).astype(BF16)
        packet_ref[1, :, cols] = (relu_pre * relu_pre).astype(BF16)


def forward(same, mine, theirs, weights, first):
    count = len(mine)
    _, rows, part = mine[0].shape
    hidden = weights[0].shape[1]
    tokens = count * rows
    made = [
        jax.ShapeDtypeStruct((2, tokens, hidden + part), BF16),
        jax.ShapeDtypeStruct((2, tokens, part), BF16),
    ]
    scratch = [pltpu.VMEM((2, tokens, part), BF16)]
    if first:
        made += [jax.ShapeDtypeStruct(t.shape, t.dtype) for t in weights[2:]]
        scratch += [pltpu.SemaphoreType.DMA((2, hidden // tile_of(hidden)))]
    return pl.pallas_call(
        functools.partial(forward_kernel, count, first),
        in_specs=[SMEM] + [VMEM] * (2 * count + 2) + [HBM if first else VMEM] * 2,
        out_specs=[VMEM] * len(made),
        out_shape=made,
        scratch_shapes=scratch,
        compiler_params=pltpu.CompilerParams(vmem_limit_bytes=FORWARD_MIB * MIB),
        cost_estimate=pl.CostEstimate(
            flops=8 * tokens * part * hidden, bytes_accessed=8 * part * hidden, transcendentals=0
        ),
        name="forward",
    )(same, *mine, *theirs, *weights)


def inputs_kernel(same_ref, packet_ref, up_ref, up_other, out_ref):
    _, rows, part = out_ref.shape
    tile = tile_of(part)
    pre_grad = packet_ref[0, :rows, : up_ref.shape[1]]
    same = same_ref[0]
    for held, here in ((up_ref, 1 - same), (up_other, same)):
        for at in range(0, part, tile):
            place = pl.ds(at, tile)
            out_ref[here, :, place] = dot(pre_grad, held[place, :], ((1,), (1,))).astype(BF16)


def inputs_part(same, packet, rows, held_up, other_up):
    part, hidden = held_up.shape
    return pl.pallas_call(
        inputs_kernel,
        in_specs=[SMEM] + [VMEM] * 3,
        out_specs=VMEM,
        out_shape=jax.ShapeDtypeStruct((2, rows, part), BF16),
        compiler_params=pltpu.CompilerParams(vmem_limit_bytes=FORWARD_MIB * MIB),
        cost_estimate=pl.CostEstimate(
            flops=4 * rows * part * hidden, bytes_accessed=4 * part * hidden, transcendentals=0
        ),
        name="inputs_part",
    )(same, packet, held_up, other_up)


def grads_of(pieces, cols, hidden):
    def rows(which):
        parts = []
        for keep, packet, got in pieces:
            parts += [packet[which, :, cols], got[which, :, cols]]
        return jnp.concatenate(parts, axis=0)

    def tokens(which):
        parts = []
        for keep, packet, got in pieces:
            parts += [keep[which], got[which, :, hidden:]]
        return jnp.concatenate(parts, axis=0)

    return lambda: dot(tokens(0), rows(0), ((0,), (0,))), lambda: dot(rows(1), tokens(1), ((0,), (0,)))


def triples(refs, count):
    return [refs[3 * at : 3 * at + 3] for at in range(count)]


def accumulate_kernel(count, first, last, *refs):
    pieces = triples(refs, count)
    if last:
        *refs, here_ref, passed_ref, up_ref, down_ref, inputs_ref = refs

        @pl.when(pl.program_id(0) == 0)
        def _():
            inputs_ref[...] = (here_ref[0].astype(F32) + passed_ref[...].astype(F32)).astype(BF16)

    else:
        up_ref, down_ref = refs[-2:]
    up_in, down_in = (None, None) if first else refs[3 * count : 3 * count + 2]
    hidden = down_ref.shape[0] if first else down_in.shape[0]
    tile = down_ref.shape[0] if last else tile_of(hidden)

    def add(step, up_to, down_to):
        cols = pl.ds(pl.multiple_of(step * tile, tile), tile)
        up, down = grads_of(pieces, cols, hidden)
        total = up() if first else up_in[:, cols].astype(F32) + up()
        up_ref[:, up_to(cols)] = total.astype(up_ref.dtype)
        total = down() if first else down_in[cols, :].astype(F32) + down()
        down_ref[down_to(cols), :] = total.astype(down_ref.dtype)

    if last:
        add(pl.program_id(0), lambda cols: slice(None), lambda cols: slice(None))
    else:
        pl.loop(0, hidden // tile)(lambda step: add(step, lambda cols: cols, lambda cols: cols))


def accumulate(pieces, sums, last, parts):
    keep, packet, _ = pieces[0]
    tokens = sum(piece[0].shape[1] for piece in pieces)
    part = keep.shape[2]
    hidden = packet.shape[2] - part
    tile = tile_of(hidden)
    args = [array for piece in pieces for array in piece] + list(sums or ())
    if last:
        args += parts
    how = dict(
        in_specs=[VMEM] * len(args),
        out_specs=[VMEM, VMEM],
        out_shape=[
            jax.ShapeDtypeStruct((part, hidden), F32 if last else BF16),
            jax.ShapeDtypeStruct((hidden, part), F32 if last else BF16),
        ]
        + [jax.ShapeDtypeStruct(t.shape, t.dtype) for t in parts[1:] if last],
        compiler_params=pltpu.CompilerParams(vmem_limit_bytes=(12 if last else 7) * MIB),
        cost_estimate=pl.CostEstimate(
            flops=8 * tokens * part * hidden, bytes_accessed=8 * part * hidden, transcendentals=0
        ),
        name="accumulate",
    )
    if last:
        how |= dict(
            grid=(hidden // tile,),
            out_specs=[
                pl.BlockSpec((part, tile), lambda j: (0, j)),
                pl.BlockSpec((tile, part), lambda j: (j, 0)),
                pl.BlockSpec(parts[1].shape, lambda j: (0, 0)),
            ],
        )
    elif sums is not None:
        how |= dict(input_output_aliases={len(args) - 2: 0, len(args) - 1: 1})
    return pl.pallas_call(
        functools.partial(accumulate_kernel, len(pieces), sums is None, last), **how
    )(*args)


def build(mesh):
    n_rep, n_fs, _ = (mesh.shape[name] for name in ("rep", "fs", "tp"))

    def shards(inputs, cotangent, w_up, w_down):
        rows, _ = inputs.shape
        group = plan(n_rep, rows * n_fs, w_up.shape[1])
        length = group // 2
        ring = folded_ring(length)
        follows = {ring[i]: ring[(i + 1) % length] for i in range(length)}
        along = [
            (base * group + 2 * at + side, base * group + 2 * follows[at] + side)
            for base in range(n_rep // group)
            for at in range(length)
            for side in range(2)
        ]
        back = [(target, source) for source, target in along]
        across = [(place, place ^ 1) for place in range(n_rep)]
        swap = [(0, 1), (1, 0)]

        same = lax.axis_index("fs") == lax.axis_index("tp")
        flag = same.astype(jnp.int32)[None]

        far_end = length - 1 if length > 2 else None
        near = {0: jnp.stack([inputs, cotangent])}
        beside = {0: lax.ppermute(near[0], "tp", swap)}
        over = {0: lax.ppermute(near[0], "rep", across)}
        corner = {0: lax.ppermute(beside[0], "rep", across)}
        for step in range(1, length):
            near[step] = lax.ppermute(near[step - 1], "rep", along)
            if step == far_end:
                beside[step] = lax.ppermute(beside[0], "rep", back)
                over[step] = lax.ppermute(over[0], "rep", back)
                corner[step] = lax.ppermute(beside[step], "rep", across)
            else:
                beside[step] = lax.ppermute(near[step], "tp", swap)
                over[step] = lax.ppermute(near[step], "rep", across)
                corner[step] = lax.ppermute(over[step], "tp", swap)
        other_up = lax.ppermute(w_up, "fs", swap)
        other_down = lax.ppermute(w_down, "fs", swap)
        weights = (w_up, w_down, other_up, other_down)
        flag = ready(flag, w_up, w_down)
        own = [(near[k], beside[k]) for k in range(length)]
        far = [(over[k], corner[k]) for k in range(length)]
        groups = {f"o{k}": group for k, group in enumerate(own)}
        groups |= {f"f{k}": group for k, group in enumerate(far)}

        made = []
        for at, names in enumerate(CHUNKS):
            packet, keep, *more = forward(
                flag, *zip(*(groups[name] for name in names)), weights, at == 0
            )
            if at == 0:
                weights = (w_up, w_down, *more)
            made.append((keep, packet, lax.ppermute(packet, "fs", swap)))
        partial_value = inputs_part(flag, made[0][1], rows, w_up, weights[2])
        passed = lax.ppermute(partial_value[1], "tp", swap)
        sums = None
        for at, chunks in enumerate(BATCHES):
            sums = accumulate([made[k] for k in chunks], sums, at == len(BATCHES) - 1, [partial_value, passed])
        grad_up, grad_down, grad_inputs = sums

        if n_rep > group:
            sets = [[base * group + at for base in range(n_rep // group)] for at in range(group)]
            grad_up, grad_down = (
                lax.psum(t, "rep", axis_index_groups=sets) for t in (grad_up, grad_down)
            )
        return (grad_inputs, grad_up, grad_down)

    return shards


CHUNKS = (("o0",), ("o1", "f0"), ("o2", "f1", "o3"), ("f2", "f3"))
BATCHES = ((0, 1), (2,), (3,))


def solution(mesh):
    run = build(mesh)

    return jax.shard_map(
        run,
        mesh=mesh,
        in_specs=(P(("rep", "fs"), "tp"), P(("rep", "fs"), "tp"), P("fs", "tp"), P("tp", "fs")),
        out_specs=(P(("rep", "fs"), "tp"), P("fs", "tp"), P("tp", "fs")),
        check_vma=False,
    )
```
